32 devices in a mesh: kv: 8 (over z, x), tp: 4 (over y, core).
Axes of the slice: x: 2, y: 2, z: 4, core: 2. Of those that a mesh axis runs over, the one named last changes fastest.
Arguments:
- tokens: bfloat16 [96, 4096], P(None, 'kv'), may hold values from -210 to 210
- norm_gain: float32 [4096], P('kv'), may hold values from 0.1 to 1.9
- w_query: bfloat16 [4096, 4096], P('kv', 'tp'), may hold values from -1 to 1
- w_key: bfloat16 [4096, 4096], P('kv', 'tp'), may hold values from -2 to 2
- w_value: bfloat16 [4096, 4096], P('kv', 'tp'), may hold values from -0.09375 to 0.09375
- w_output: bfloat16 [4096, 4096], P('tp', 'kv'), may hold values from -0.09375 to 0.09375
- cache_keys: bfloat16 [4, 4096, 4096], P(None, 'kv', 'tp'), may hold values from -820 to 820
- cache_values: bfloat16 [4, 4096, 4096], P(None, 'kv', 'tp'), may hold values from -6 to 6
- map_lambda: float32 [64], P('tp'), may hold values from 0.3 to 0.8
- out_gain: float32 [4096], P('tp'), may hold values from 0.1 to 1.9
- parents: int32 [4, 24], replicated, may hold values from -1 to 22, as said below
- lengths: int32 [4], replicated, may hold values from 2048 to 4048, as said below
- accepted: int32 [4], replicated, may hold values from 0 to 24
Outputs:
- mixed: bfloat16 [96, 4096], P(None, 'kv')
- new_keys: bfloat16 [4, 4096, 4096], P(None, 'kv', 'tp')
- new_values: bfloat16 [4, 4096, 4096], P(None, 'kv', 'tp')
The draws below stay inside these ranges and needn't reach their ends.
Inputs may be any that keep to these rules, and one draw needn't show every extreme that they name: parents[b, j] lies between -1 and j - 1. `lengths`: some sequence has exactly the largest value.
All inputs are finite; a program needn't handle non-finite values.
Results may differ from the reference program's by a relative error of at most 0.029.
Values may be sent and summed in bfloat16 or wider, within the bound.
A program may use at most 128 MiB of HBM per device.

```python
import math
import jax
import jax.numpy as jnp
from jax import lax

D = 4096
HEADS = 64
HEAD = 64
QK = 32
SEQS = 4
POS_DEV = 512
PROP = 24
CACHE = 4096
ROWS = 96
N_KV = 8
N_TP = 4


def draw_tokens(key, part):
    column_rise = jnp.arange(D, dtype=jnp.float32) / (D - 1)
    shared_part = 0.8 ** 0.5
    own_part = 0.2 ** 0.5
    common = jax.random.normal(jax.random.fold_in(key, 11), (SEQS, 1, D), jnp.float32)
    own = jax.random.normal(key, (SEQS, PROP, D), jnp.float32)
    mixture = jnp.clip(shared_part * common + own_part * own, -6.0, 6.0).reshape(ROWS, D)
    values = mixture * jnp.exp(column_rise * 1.1)
    return values.astype(jnp.bfloat16)


def query_matrix(key):
    base = jnp.clip(jax.random.normal(jax.random.fold_in(key, 21), (D, HEADS * HEAD), jnp.float32), -6.0, 6.0)
    return base * D ** (-0.5)


def draw_w_query(key, part):
    return query_matrix(key).astype(jnp.bfloat16)


def draw_w_key(key, part):
    coupling = math.log(1.6 * CACHE) / math.sqrt(QK)
    noise = jnp.clip(jax.random.normal(jax.random.fold_in(key, 22), (D, HEADS * HEAD), jnp.float32), -6.0, 6.0)
    values = coupling * query_matrix(key) + noise * D ** (-0.5)
    return values.astype(jnp.bfloat16)


def draw_cache_keys(key, part):
    values = 1.7 * jnp.clip(jax.random.normal(key, (SEQS, CACHE, HEADS * HEAD), jnp.float32), -6.0, 6.0)
    return values.astype(jnp.bfloat16)


def draw_parents(key, part):
    limits = jnp.arange(PROP, dtype=jnp.int32)
    return jax.random.randint(key, (SEQS, PROP), -1, limits[None, :]).astype(jnp.int32)


def draw_lengths(key, part):
    drawn = jax.random.randint(key, (SEQS,), CACHE // 2, CACHE - 2 * PROP + 1)
    chosen = jax.random.randint(jax.random.fold_in(key, 1), (), 0, SEQS)
    return drawn.at[chosen].set(CACHE - 2 * PROP).astype(jnp.int32)


def with_ends(array, stream_key, least, high):
    longest = array.shape.index(max(array.shape))
    spots = []
    for shift in (0, 1):
        where = [jax.random.randint(jax.random.fold_in(stream_key, axis), (), 0, length) for axis, length in enumerate(array.shape)]
        where[longest] = (where[longest] + shift) % array.shape[longest]
        spots.append(tuple(where))
    return array.at[spots[0]].set(least).at[spots[1]].set(high)


def block_levels(own_key, extent, shards, smallest, largest):
    factor_of = 1.0
    for position, shards_of in shards:
        heights = jax.random.uniform(jax.random.fold_in(jax.random.fold_in(own_key, 6), position), (shards_of,), jnp.float32, smallest / len(shards), largest / len(shards))
        factor_of = factor_of * jnp.repeat(jnp.exp(heights), extent[position] // shards_of).reshape((-1,) + (1,) * (len(extent) - 1 - position))
    return factor_of


def bell_draw(own_key, shape, scale, reach, split=(), kind=jnp.bfloat16):
    values = scale * jax.random.normal(own_key, shape, jnp.float32)
    if split:
        values = values * block_levels(own_key, shape, split, -0.22, 0.18)
    return jnp.clip(values, -reach, reach).astype(kind)


def setup_inputs(seed: int = 0) -> dict:
    keys = jax.random.split(jax.random.key(seed), 14)
    tokens = draw_tokens(jax.random.fold_in(keys[13], 71), 0)
    norm_gain = jnp.clip(1.0 + 0.18 * jax.random.normal(keys[1], (D,), jnp.float32), 0.1, 1.9)
    w_query = draw_w_query(jax.random.fold_in(keys[13], 71), 0)
    w_key = draw_w_key(jax.random.fold_in(keys[13], 71), 0)
    w_value = bell_draw(keys[4], (D, HEADS * HEAD), D ** -0.5, 0.09375, ((0, 8), (1, 4)))
    w_output = bell_draw(keys[5], (HEADS * HEAD, D), (HEADS * HEAD) ** -0.5, 0.09375, ((0, 4), (1, 8)))
    cache_keys = draw_cache_keys(jax.random.fold_in(keys[13], 71), 0)
    cache_values = bell_draw(keys[7], (SEQS, CACHE, HEADS * HEAD), 1.0, 6.0, ((1, 8), (2, 4)))
    map_lambda = jnp.clip(0.3 + 0.5 * jax.random.uniform(keys[8], (HEADS,), jnp.float32) ** block_levels(keys[8], (HEADS,), ((0, 4),), -0.2, 0.2), 0.3, 0.8)
    out_gain = jnp.clip(1.0 + 0.18 * jax.random.normal(keys[9], (HEADS * HEAD,), jnp.float32), 0.1, 1.9)
    parents = draw_parents(jax.random.fold_in(keys[13], 71), 0)
    lengths = draw_lengths(jax.random.fold_in(keys[13], 71), 0)
    accepted = with_ends(jax.random.randint(keys[12], (SEQS,), 0, PROP + 1), jax.random.fold_in(keys[12], 1), 0, PROP).astype(jnp.int32)
    return dict(tokens=tokens, norm_gain=norm_gain, w_query=w_query, w_key=w_key, w_value=w_value, w_output=w_output, cache_keys=cache_keys, cache_values=cache_values, map_lambda=map_lambda, out_gain=out_gain, parents=parents, lengths=lengths, accepted=accepted)


epsilon = 1e-05
masked_low = -1e+30

def ancestry(parents):
    count = parents.shape[1]
    places = jnp.arange(count, dtype=jnp.int32)
    parent_links = (parents[:, :, None] == places[None, None, :]).astype(jnp.float32)
    identity = jnp.eye(count, dtype=jnp.float32)[None]

    def extend(turn_index, reached):
        return jnp.minimum(1.0, identity + jnp.einsum('bji,bik->bjk', parent_links, reached))
    reached = lax.fori_loop(0, count, extend, jnp.broadcast_to(identity, parent_links.shape))
    return reached > 0.5

def reference(tokens, norm_gain, w_query, w_key, w_value, w_output, cache_keys, cache_values, map_lambda, out_gain, parents, lengths, accepted):
    f32 = jnp.float32
    bf16 = jnp.bfloat16
    tokens_wide = tokens.astype(f32)
    norm_factor = lax.rsqrt(lax.optimization_barrier(jnp.mean(tokens_wide * tokens_wide, axis=1, keepdims=True)) + epsilon)
    gained = (tokens_wide * norm_gain).astype(bf16)

    def projection(weight_matrix):
        return (jnp.dot(gained, weight_matrix, preferred_element_type=f32) * norm_factor).astype(bf16)
    queries = projection(w_query)
    keys_flat = projection(w_key)
    values_flat = projection(w_value)
    query_heads = queries.astype(f32).reshape(SEQS, PROP, HEADS, 2, QK)
    key_heads = keys_flat.astype(f32).reshape(SEQS, PROP, HEADS, 2, QK)
    value_heads = values_flat.reshape(SEQS, PROP, HEADS, HEAD)
    start = lengths + accepted
    score_scale = QK ** (-0.5)

    def cache_block(block_index):
        begin = (block_index * POS_DEV).astype(jnp.int32)
        block_keys = lax.dynamic_slice_in_dim(cache_keys, begin, POS_DEV, 1).astype(f32)
        block_keys = block_keys.reshape(SEQS, POS_DEV, HEADS, 2, QK)
        block_vals = lax.dynamic_slice_in_dim(cache_values, begin, POS_DEV, 1).astype(f32)
        block_vals = block_vals.reshape(SEQS, POS_DEV, HEADS, HEAD)
        positions = begin + jnp.arange(POS_DEV, dtype=jnp.int32)
        visible = (positions[None, :] < start[:, None])[:, None, None, None, :]
        scores = jnp.einsum('bqhmd,bkhmd->bmhqk', query_heads, block_keys) * score_scale
        block_max = lax.optimization_barrier(jnp.max(jnp.where(visible, scores, masked_low), axis=-1))
        block_weight = jnp.where(visible, jnp.exp(scores - block_max[..., None]), 0.0)
        block_total = lax.optimization_barrier(jnp.sum(block_weight, axis=-1))
        rounded = block_weight.astype(bf16).astype(f32)
        block_values = jnp.einsum('bmhqk,bkhd->bmhqd', rounded, block_vals).astype(bf16)
        return (block_max, block_total, block_values)
    maxima, totals, values = lax.map(cache_block, jnp.arange(N_KV, dtype=jnp.int32))
    cache_max = lax.optimization_barrier(jnp.max(maxima, axis=0))
    factors = jnp.exp(maxima - cache_max[None])
    cache_total = lax.optimization_barrier(jnp.sum(totals * factors, axis=0))
    cache_sum = lax.optimization_barrier(jnp.sum(values.astype(f32) * factors[..., None], axis=0))
    lineage = ancestry(parents)[:, None, None, :, :]
    self_scores = jnp.einsum('bqhmd,bjhmd->bmhqj', query_heads, key_heads) * score_scale
    self_max = lax.optimization_barrier(jnp.max(jnp.where(lineage, self_scores, masked_low), axis=-1))
    top = jnp.maximum(cache_max, self_max)
    self_weight = jnp.where(lineage, jnp.exp(self_scores - top[..., None]), 0.0)
    carried = jnp.exp(cache_max - top)
    denominator = cache_total * carried + lax.optimization_barrier(jnp.sum(self_weight, axis=-1))
    self_values = jnp.einsum('bmhqj,bjhd->bmhqd', self_weight.astype(bf16).astype(f32), value_heads.astype(f32))
    attended = (cache_sum * carried[..., None] + self_values) / denominator[..., None]
    difference = attended[:, 0] - map_lambda[None, :, None, None] * attended[:, 1]
    gains = out_gain.reshape(HEADS, HEAD)[None, :, None, :]
    normed = difference * lax.rsqrt(lax.optimization_barrier(jnp.mean(difference * difference, axis=-1, keepdims=True)) + epsilon) * gains
    normed = jnp.transpose(normed, (0, 2, 1, 3)).reshape(ROWS, HEADS * HEAD).astype(bf16)
    group = HEADS // N_TP
    pieces = normed.reshape(ROWS, N_TP, group * HEAD).astype(f32)
    weight_groups = w_output.reshape(N_TP, group * HEAD, D).astype(f32)
    partials = jnp.einsum('rgc,gcd->grd', pieces, weight_groups).astype(bf16)
    partials = lax.optimization_barrier(partials).astype(f32)
    mixed = lax.optimization_barrier(jnp.sum(partials, axis=0)).astype(bf16)

    def place(cache_row, new_rows, begin):
        return lax.dynamic_update_slice(cache_row, new_rows, (begin, jnp.int32(0)))
    new_keys = jax.vmap(place)(cache_keys, keys_flat.reshape(SEQS, PROP, HEADS * HEAD), start)
    new_values = jax.vmap(place)(cache_values, values_flat.reshape(SEQS, PROP, HEADS * HEAD), start)
    return (mixed, new_keys, new_values)
```

```python
import functools

import jax
import jax.numpy as jnp
from jax import lax
from jax.experimental import pallas as pl
from jax.experimental.pallas import tpu as pltpu
from jax.sharding import PartitionSpec as P

HEAD = 64
QK = 32
LANES = 128
epsilon = 1e-05
masked_low = -1e30
MESH = pl.DeviceIdType.MESH
f32 = jnp.float32
bf16 = jnp.bfloat16


def iota(shape, dim):
    return lax.broadcasted_iota(jnp.int32, shape, dim)


def greet(axes):
    barrier = pltpu.get_barrier_semaphore()
    count = 0
    for axis, n in axes:
        me = lax.axis_index(axis)
        for k in range(1, n):
            pl.semaphore_signal(
                barrier, inc=1, device_id={axis: lax.rem(me + k, n)}, device_id_type=MESH
            )
            count += 1
    return barrier, count


def remote(src, dst, send_sem, recv_sem, axis, to):
    return pltpu.make_async_remote_copy(
        src_ref=src,
        dst_ref=dst,
        send_sem=send_sem,
        recv_sem=recv_sem,
        device_id={axis: to},
        device_id_type=MESH,
    )


def project_kernel(
    n, cols, features, tok_ref, gain_ref, wq_ref, wk_ref, wv_ref, out_ref,
    send, recv, sq_send, sq_recv, s_send, s_recv, q_send, q_recv, g_send, g_recv,
):
    me = lax.axis_index("kv")
    groups = n // cols
    rows = tok_ref.shape[0]
    part = rows // groups
    barrier, count = greet((("kv", n),))
    wide = tok_ref[...].astype(f32)
    gained = (wide * gain_ref[...]).astype(bf16)
    square = jnp.sum(wide * wide, axis=1, keepdims=True)
    diagonal = iota((rows, LANES), 0) == iota((rows, LANES), 1)
    as_row = jnp.sum(jnp.where(diagonal, square, 0.0), axis=0, keepdims=True)
    sq_send[...] = jnp.broadcast_to(as_row, sq_send.shape)
    for i, ref in enumerate((wq_ref, wk_ref, wv_ref)):
        product = jnp.dot(gained, ref[...], preferred_element_type=f32)
        for c in range(cols):
            for r in range(groups):
                send[c * groups + r, :, i * LANES : (i + 1) * LANES] = product[
                    r * part : (r + 1) * part, c * LANES : (c + 1) * LANES
                ].astype(bf16)
    pl.semaphore_wait(barrier, count)
    copies = []
    for k in range(1, n):
        to = lax.rem(me + k, n)
        copies.append(remote(sq_send, sq_recv.at[k], q_send.at[k], q_recv.at[k], "kv", to))
        copies.append(remote(send.at[to], recv.at[k], s_send.at[k], s_recv.at[k], "kv", to))
    for copy in copies:
        copy.start()
    total = send[me].astype(f32)
    squares = sq_send[...]
    for k in range(1, n):
        copies[2 * k - 2].wait()
        squares = squares + sq_recv[k]
    for k in range(1, n):
        copies[2 * k - 1].wait()
        total = total + recv[k].astype(f32)
    first = lax.rem(me, groups) * part
    picked = iota((part, LANES), 0) + first == iota((part, LANES), 1)
    mean = jnp.sum(jnp.where(picked, squares[0:1], 0.0), axis=1, keepdims=True) / features
    out_ref[me] = (total * lax.rsqrt(mean + epsilon)).astype(bf16)
    copies = []
    for k in range(1, n):
        to = lax.rem(me + k, n)
        copies.append(remote(out_ref.at[me], out_ref.at[me], g_send.at[k], g_recv.at[k], "kv", to))
    for copy in copies:
        copy.start()
    for copy in copies:
        copy.wait()


def cache_kernel(
    groups, prop, rel_ref, ga_ref, keys_hbm, vals_hbm, nk_hbm, nv_hbm, bv_ref, st_ref,
    kbuf, vbuf, k_in, v_in, k_out, v_out,
):
    seqs, length, width = kbuf.shape
    cols = width // LANES
    per = seqs // groups
    both = 2 * prop
    loads = []
    for b in range(seqs):
        loads.append(
            (
                pltpu.make_async_copy(keys_hbm.at[b], kbuf.at[b], k_in.at[b]),
                pltpu.make_async_copy(vals_hbm.at[b], vbuf.at[b], v_in.at[b]),
            )
        )
        loads[b][0].start()
        loads[b][1].start()
    st_ref[...] = jnp.zeros_like(st_ref)
    stores = []
    window = 48
    lane = iota((1, LANES), 1)
    wide_lane = iota((1, 2 * LANES), 1)
    scale = QK ** (-0.5)
    for b in range(seqs):
        r, inner = b // per, b % per
        begin = inner * prop
        rel = rel_ref[b]

        def fresh(which):
            return jnp.concatenate(
                [
                    ga_ref[c * groups + r, begin : begin + prop, which * LANES : (which + 1) * LANES]
                    for c in range(cols)
                ],
                axis=1,
            )

        base = jnp.clip((rel // 16) * 16, 0, length - window)
        at = pl.ds(pl.multiple_of(base, 16), window)
        slot = iota((window, prop), 0) + base - rel
        placing = (slot == iota((window, prop), 1)).astype(bf16)
        slot_col = iota((window, 1), 0) + base - rel
        inside = (slot_col >= 0) & (slot_col < prop)
        for which, buf, pos in ((1, kbuf, 0), (2, vbuf, 1)):
            loads[b][pos].wait()
            moved = jnp.dot(placing, fresh(which), preferred_element_type=f32)
            old = buf[b, at, :].astype(f32)
            buf[b, at, :] = jnp.where(inside, moved, old).astype(bf16)
        stores.append(pltpu.make_async_copy(kbuf.at[b], nk_hbm.at[b], k_out.at[b]))
        stores.append(pltpu.make_async_copy(vbuf.at[b], nv_hbm.at[b], v_out.at[b]))
        stores[-2].start()
        stores[-1].start()
        queries = fresh(0)
        visible = iota((1, length), 1) < rel
        for g in range(width // (2 * LANES)):
            span = slice(g * 2 * LANES, (g + 1) * 2 * LANES)
            part = queries[:, span].astype(f32)
            spread = jnp.concatenate(
                [jnp.where(wide_lane // QK == i, part, 0.0) for i in range(2 * LANES // QK)], axis=0
            ).astype(bf16)
            scores = lax.dot_general(
                spread, kbuf[b, :, span], (((1,), (1,)), ((), ())), preferred_element_type=f32
            )
            scores = jnp.where(visible, scores * scale, masked_low)
            largest = jnp.max(scores, axis=1, keepdims=True)
            weight = jnp.where(visible, jnp.exp(scores - largest), 0.0)
            total = jnp.sum(weight, axis=1, keepdims=True)
            summed = jnp.dot(weight.astype(bf16), vbuf[b, :, span], preferred_element_type=f32)
            merged = jnp.zeros((both, 2 * LANES), f32)
            for h in range(2 * LANES // HEAD):
                piece = slice(h * both, (h + 1) * both)
                merged = jnp.where(wide_lane // HEAD == h, summed[piece], merged)
                c = g * 2 + h // 2
                first = inner * 4 + h % 2
                stat = st_ref[c, r]
                stat = jnp.where(lane == first, largest[piece], stat)
                st_ref[c, r] = jnp.where(lane == first + 2, total[piece], stat)
            merged = merged.astype(bf16)
            for half in range(2):
                bv_ref[g * 2 + half, r, inner * both : (inner + 1) * both, :] = merged[
                    :, half * LANES : (half + 1) * LANES
                ]
    for copy in stores:
        copy.wait()


def merge_kernel(
    n, t, cols, seqs, prop, parent_ref, lam_ref, gain_ref, ga_ref, bv_ref, st_ref, wo_ref, out_ref,
    bv_recv, st_recv, norm_all, out_part, out_recv,
    b_send, b_recv, s_send, s_recv, g_send, g_recv, t_send, t_recv,
):
    me = lax.axis_index("kv")
    mine = lax.axis_index("tp")
    groups = n // cols
    per = seqs // groups
    part = per * prop
    both = 2 * prop
    barrier, count = greet((("kv", n), ("tp", t)))
    pl.semaphore_wait(barrier, count)
    copies = []
    for k in range(1, n):
        to = lax.rem(me + k, n)
        c, r = to // groups, lax.rem(to, groups)
        copies.append(remote(st_ref.at[c, r], st_recv.at[k], s_send.at[k], s_recv.at[k], "kv", to))
        copies.append(remote(bv_ref.at[c, r], bv_recv.at[k], b_send.at[k], b_recv.at[k], "kv", to))
    for copy in copies:
        copy.start()
    col, row = me // groups, lax.rem(me, groups)
    lane = iota((1, LANES), 1)
    scale = QK ** (-0.5)
    shape = (part, part)
    target = parent_ref[...] + (iota((part, 1), 0) // prop) * prop
    link = (parent_ref[...] >= 0) & (target == iota(shape, 1))
    eye = iota(shape, 0) == iota(shape, 1)
    reach = jnp.where(link | eye, 1.0, 0.0)
    power = 1
    while power < prop:
        reach = jnp.minimum(
            jnp.dot(reach.astype(bf16), reach.astype(bf16), preferred_element_type=f32), 1.0
        )
        power *= 2
    lineage = jnp.concatenate([reach] * 4, axis=0) > 0.5
    own = ga_ref[me]
    query = own[:, :LANES].astype(f32)
    spread = jnp.concatenate(
        [jnp.where(lane // QK == i, query, 0.0) for i in range(4)], axis=0
    ).astype(bf16)
    scores = lax.dot_general(
        spread, own[:, LANES : 2 * LANES], (((1,), (1,)), ((), ())), preferred_element_type=f32
    )
    scores = jnp.where(lineage, scores * scale, masked_low)
    top = jnp.max(scores, axis=1, keepdims=True)
    weight = jnp.where(lineage, jnp.exp(scores - top), 0.0)
    total = jnp.sum(weight, axis=1, keepdims=True)
    summed = jnp.dot(weight.astype(bf16), own[:, 2 * LANES :], preferred_element_type=f32)
    low = lane < HEAD

    def laid(array):
        pieces = []
        for b in range(per):
            for m in range(2):
                s0 = slice(m * part + b * prop, m * part + (b + 1) * prop)
                s1 = slice((2 + m) * part + b * prop, (2 + m) * part + (b + 1) * prop)
                pieces.append(jnp.where(low, array[s0], array[s1]))
        return jnp.concatenate(pieces, axis=0)

    tops = [laid(top)]
    totals = [laid(total)]
    sums = [laid(summed)]

    def take(stats, values):
        for which, into in ((0, tops), (2, totals)):
            into.append(
                jnp.concatenate(
                    [
                        jnp.where(
                            low,
                            stats[:, b * 4 + which : b * 4 + which + 1],
                            stats[:, b * 4 + which + 1 : b * 4 + which + 2],
                        )
                        for b in range(per)
                    ],
                    axis=0,
                )
            )
        sums.append(values.astype(f32))

    take(st_ref[col, row], bv_ref[col, row])
    for copy in copies:
        copy.wait()
    for k in range(1, n):
        take(st_recv[k], bv_recv[k])
    highest = functools.reduce(jnp.maximum, tops)
    denominator = jnp.zeros_like(highest)
    numerator = jnp.zeros_like(highest)
    for a, b, c in zip(tops, totals, sums):
        factor = jnp.exp(a - highest)
        denominator = denominator + b * factor
        numerator = numerator + c * factor
    attended = numerator / denominator
    lam = lam_ref[pl.ds(col, 1), :]
    gain = gain_ref[pl.ds(col, 1), :]
    difference = jnp.concatenate(
        [
            attended[b * both : b * both + prop] - lam * attended[b * both + prop : (b + 1) * both]
            for b in range(per)
        ],
        axis=0,
    )
    squared = difference * difference
    one = jnp.sum(jnp.where(low, squared, 0.0), axis=1, keepdims=True)
    two = jnp.sum(jnp.where(low, 0.0, squared), axis=1, keepdims=True)
    mean = jnp.where(low, one, two) / HEAD
    norm_all[me] = (difference * lax.rsqrt(mean + epsilon) * gain).astype(bf16)
    copies = []
    for k in range(1, n):
        to = lax.rem(me + k, n)
        copies.append(
            remote(norm_all.at[me], norm_all.at[me], g_send.at[k], g_recv.at[k], "kv", to)
        )
    for copy in copies:
        copy.start()
    for copy in copies:
        copy.wait()
    normed = jnp.concatenate(
        [
            jnp.concatenate([norm_all[c * groups + r] for r in range(groups)], axis=0)
            for c in range(cols)
        ],
        axis=1,
    )
    out_part[...] = jnp.dot(normed, wo_ref[...], preferred_element_type=f32).astype(bf16)
    copies = []
    for k in range(1, t):
        to = lax.rem(mine + k, t)
        copies.append(remote(out_part, out_recv.at[k], t_send.at[k], t_recv.at[k], "tp", to))
    for copy in copies:
        copy.start()
    mixed = out_part[...].astype(f32)
    for k in range(1, t):
        copies[k - 1].wait()
        mixed = mixed + out_recv[k].astype(f32)
    out_ref[...] = mixed.astype(bf16)


def local(
    n, t, tokens, norm_gain, w_query, w_key, w_value, w_output, cache_keys, cache_values,
    map_lambda, out_gain, parents, lengths, accepted,
):
    rows, depth = tokens.shape
    seqs, length, width = cache_keys.shape
    prop = rows // seqs
    both = 2 * prop
    cols = min(n, width // LANES)
    groups = n // cols
    part = rows // groups
    per = seqs // groups
    vmem = pl.BlockSpec(memory_space=pltpu.VMEM)
    smem = pl.BlockSpec(memory_space=pltpu.SMEM)
    hbm = pl.BlockSpec(memory_space=pl.ANY)
    dma = pltpu.SemaphoreType.DMA
    gathered = pl.pallas_call(
        functools.partial(project_kernel, n, cols, depth * n),
        name="project",
        out_shape=jax.ShapeDtypeStruct((n, part, 3 * LANES), bf16),
        in_specs=[vmem] * 5,
        out_specs=vmem,
        scratch_shapes=[
            pltpu.VMEM((n, part, 3 * LANES), bf16),
            pltpu.VMEM((n, part, 3 * LANES), bf16),
            pltpu.VMEM((8, LANES), f32),
            pltpu.VMEM((n, 8, LANES), f32),
        ]
        + [dma((n,))] * 6,
        compiler_params=pltpu.CompilerParams(collective_id=0, has_side_effects=True),
    )(tokens, norm_gain[None], w_query, w_key, w_value)
    start = lengths + accepted
    relative = (start - lax.axis_index("kv") * length).astype(jnp.int32)
    new_keys, new_values, block_values, stats = pl.pallas_call(
        functools.partial(cache_kernel, groups, prop),
        name="cache",
        out_shape=(
            jax.ShapeDtypeStruct(cache_keys.shape, bf16),
            jax.ShapeDtypeStruct(cache_values.shape, bf16),
            jax.ShapeDtypeStruct((cols, groups, per * both, LANES), bf16),
            jax.ShapeDtypeStruct((cols, groups, both, LANES), f32),
        ),
        in_specs=[smem, vmem, hbm, hbm],
        out_specs=(hbm, hbm, vmem, vmem),
        scratch_shapes=[
            pltpu.VMEM(cache_keys.shape, bf16),
            pltpu.VMEM(cache_values.shape, bf16),
        ]
        + [dma((seqs,))] * 4,
    )(relative, gathered, cache_keys, cache_values)
    first = lax.rem(lax.axis_index("kv"), groups) * per
    own_parents = lax.dynamic_slice_in_dim(parents, first, per, 0).reshape(part, 1)
    mixed = pl.pallas_call(
        functools.partial(merge_kernel, n, t, cols, seqs, prop),
        name="merge",
        out_shape=jax.ShapeDtypeStruct((rows, w_output.shape[1]), bf16),
        in_specs=[vmem] * 7,
        out_specs=vmem,
        scratch_shapes=[
            pltpu.VMEM((n, per * both, LANES), bf16),
            pltpu.VMEM((n, both, LANES), f32),
            pltpu.VMEM((n, part, LANES), bf16),
            pltpu.VMEM((rows, w_output.shape[1]), bf16),
            pltpu.VMEM((t, rows, w_output.shape[1]), bf16),
        ]
        + [dma((n,))] * 6
        + [dma((t,))] * 2,
        compiler_params=pltpu.CompilerParams(collective_id=1, has_side_effects=True),
    )(
        own_parents,
        jnp.repeat(map_lambda, HEAD).reshape(cols, LANES),
        out_gain.reshape(cols, LANES),
        gathered,
        block_values,
        stats,
        w_output,
    )
    return (mixed, new_keys, new_values)


def solution(mesh):
    placed = (
        P(None, "kv"),
        P("kv"),
        P("kv", "tp"),
        P("kv", "tp"),
        P("kv", "tp"),
        P("tp", "kv"),
        P(None, "kv", "tp"),
        P(None, "kv", "tp"),
        P("tp"),
        P("tp"),
        P(),
        P(),
        P(),
    )
    return jax.shard_map(
        functools.partial(local, mesh.shape["kv"], mesh.shape["tp"]),
        mesh=mesh,
        in_specs=placed,
        out_specs=(P(None, "kv"), P(None, "kv", "tp"), P(None, "kv", "tp")),
        check_vma=False,
    )
```

```python
import functools

import jax
import jax.numpy as jnp
from jax import lax
from jax.experimental import pallas as pl
from jax.experimental.pallas import tpu as pltpu
from jax.sharding import PartitionSpec as P

HEAD = 64
QK = 32
LANES = 128
epsilon = 1e-05
masked_low = -1e30
MESH = pl.DeviceIdType.MESH
f32 = jnp.float32
bf16 = jnp.bfloat16


def iota(shape, dim):
    return lax.broadcasted_iota(jnp.int32, shape, dim)


def greet(axes):
    barrier = pltpu.get_barrier_semaphore()
    count = 0
    for axis, n in axes:
        me = lax.axis_index(axis)
        for k in range(1, n):
            pl.semaphore_signal(
                barrier, inc=1, device_id={axis: lax.rem(me + k, n)}, device_id_type=MESH
            )
            count += 1
    return barrier, count


def remote(src, dst, send_sem, recv_sem, axis, to):
    return pltpu.make_async_remote_copy(
        src_ref=src,
        dst_ref=dst,
        send_sem=send_sem,
        recv_sem=recv_sem,
        device_id={axis: to},
        device_id_type=MESH,
    )


def main_kernel(
    n, t, cols, seqs, prop, features,
    tok_ref, gain_ref, lam_ref, out_gain_ref, parent_ref, len_ref, acc_ref,
    wq_hbm, wk_hbm, wv_hbm, wo_hbm, keys_hbm, vals_hbm,
    out_ref, kv_ref,
    wbuf, wo_buf, kbuf, vbuf, q_part, q_recv, q_all, kv_part, kv_recv, sq_part, sq_recv,
    bv, bv_recv, st, st_part, st_recv, norm_all, out_part, out_recv,
    w_in, k_in, v_in, sq_s, sq_r, q_s, q_r, qa_s, qa_r, kv_s, kv_r, ka_s, ka_r,
    b_s, b_r, st_s, st_r, g_s, g_r, t_s, t_r,
):
    me = lax.axis_index("kv")
    mine = lax.axis_index("tp")
    groups = n // cols
    rows = tok_ref.shape[0]
    part = rows // groups
    per = seqs // groups
    both = 2 * prop
    _, length, width = kbuf.shape
    scale = QK ** (-0.5)
    peers = [lax.rem(me + k, n) for k in range(1, n)]
    barrier, count = greet((("kv", n), ("tp", t)))
    weights = [
        pltpu.make_async_copy(src, dst, w_in.at[i])
        for i, (src, dst) in enumerate(
            ((wq_hbm, wbuf.at[0]), (wk_hbm, wbuf.at[1]), (wv_hbm, wbuf.at[2]), (wo_hbm, wo_buf))
        )
    ]
    loads = []
    for b in range(seqs):
        loads.append(pltpu.make_async_copy(keys_hbm.at[b], kbuf.at[b], k_in.at[b]))
        loads.append(pltpu.make_async_copy(vals_hbm.at[b], vbuf.at[b], v_in.at[b]))
    for copy in weights + loads:
        copy.start()

    wide = tok_ref[...].astype(f32)
    square = jnp.sum(wide * wide, axis=1, keepdims=True)
    diagonal = iota((rows, LANES), 0) == iota((rows, LANES), 1)
    as_row = jnp.sum(jnp.where(diagonal, square, 0.0), axis=0, keepdims=True)
    sq_part[...] = jnp.broadcast_to(as_row, sq_part.shape)
    gained = (wide * gain_ref[...]).astype(bf16)

    def products(which, into, at):
        weights[which].wait()
        product = jnp.dot(gained, wbuf[which], preferred_element_type=f32)
        for c in range(cols):
            for r in range(groups):
                into[c * groups + r, :, at : at + LANES] = product[
                    r * part : (r + 1) * part, c * LANES : (c + 1) * LANES
                ].astype(bf16)

    products(0, q_part, 0)
    pl.semaphore_wait(barrier, count)
    sq_copies, q_copies = [], []
    for k, to in enumerate(peers):
        sq_copies.append(remote(sq_part, sq_recv.at[k], sq_s.at[k], sq_r.at[k], "kv", to))
        q_copies.append(remote(q_part.at[to], q_recv.at[k], q_s.at[k], q_r.at[k], "kv", to))
    for copy in sq_copies + q_copies:
        copy.start()
    products(1, kv_part, 0)
    products(2, kv_part, LANES)
    squares = sq_part[...]
    for k in range(n - 1):
        sq_copies[k].wait()
        squares = squares + sq_recv[k]
    first = lax.rem(me, groups) * part
    picked = iota((part, LANES), 0) + first == iota((part, LANES), 1)
    mean = jnp.sum(jnp.where(picked, squares[0:1], 0.0), axis=1, keepdims=True) / features
    factor = lax.rsqrt(mean + epsilon)
    total = q_part[me].astype(f32)
    for k in range(n - 1):
        q_copies[k].wait()
        total = total + q_recv[k].astype(f32)
    q_all[me] = (total * factor).astype(bf16)
    gathers, kv_copies = [], []
    for k, to in enumerate(peers):
        gathers.append(remote(q_all.at[me], q_all.at[me], qa_s.at[k], qa_r.at[k], "kv", to))
        kv_copies.append(remote(kv_part.at[to], kv_recv.at[k], kv_s.at[k], kv_r.at[k], "kv", to))
    for copy in gathers + kv_copies:
        copy.start()

    lane = iota((1, LANES), 1)
    low = lane < HEAD
    own_first = lax.rem(me, groups) * per
    small_eye = iota((prop, prop), 0) == iota((prop, prop), 1)
    parent_rows = []
    for b in range(per):
        line = parent_ref[pl.ds(own_first + b, 1), :]
        parent_rows.append(
            jnp.sum(jnp.where(small_eye, line, 0), axis=1, keepdims=True)
        )
    parent = jnp.concatenate(parent_rows, axis=0)
    shape = (part, part)
    target = jnp.concatenate([p + b * prop for b, p in enumerate(parent_rows)], axis=0)
    link = (parent >= 0) & (target == iota(shape, 1))
    reach = jnp.where(link | (iota(shape, 0) == iota(shape, 1)), 1.0, 0.0)
    power = 1
    while power < prop:
        reach = jnp.minimum(
            jnp.dot(reach.astype(bf16), reach.astype(bf16), preferred_element_type=f32), 1.0
        )
        power *= 2
    lineage = jnp.concatenate([reach] * 4, axis=0) > 0.5
    st[...] = jnp.zeros_like(st)

    for copy in gathers:
        copy.wait()
    wide_lane = iota((1, 2 * LANES), 1)
    b_copies = []
    pieces = seqs if groups == 1 else 1
    tall = per * both // pieces

    def send_piece(piece):
        for k, to in enumerate(peers):
            c, r = to // groups, lax.rem(to, groups)
            span = pl.ds(piece * tall, tall)
            copy = remote(
                bv.at[c, r, span], bv_recv.at[k, span], b_s.at[k, piece], b_r.at[k, piece], "kv", to
            )
            copy.start()
            b_copies.append(copy)

    for b in range(seqs):
        r, inner = b // per, b % per
        begin = inner * prop
        rel = len_ref[b] + acc_ref[b] - me * length
        visible = iota((1, length), 1) < rel
        loads[2 * b].wait()
        loads[2 * b + 1].wait()
        for g in range(width // (2 * LANES)):
            span = slice(g * 2 * LANES, (g + 1) * 2 * LANES)
            query = jnp.concatenate(
                [
                    q_all[c * groups + r].astype(f32)[begin : begin + prop]
                    for c in (2 * g, 2 * g + 1)
                ],
                axis=1,
            )
            spread = jnp.concatenate(
                [jnp.where(wide_lane // QK == i, query, 0.0) for i in range(2 * LANES // QK)],
                axis=0,
            ).astype(bf16)
            scores = lax.dot_general(
                spread, kbuf[b, :, span], (((1,), (1,)), ((), ())), preferred_element_type=f32
            )
            scores = jnp.where(visible, scores * scale, masked_low)
            largest = jnp.max(scores, axis=1, keepdims=True)
            weight = jnp.where(visible, jnp.exp(scores - largest), 0.0)
            total = jnp.sum(weight, axis=1, keepdims=True)
            summed = jnp.dot(weight.astype(bf16), vbuf[b, :, span], preferred_element_type=f32)
            merged = jnp.zeros((both, 2 * LANES), f32)
            for h in range(2 * LANES // HEAD):
                piece = slice(h * both, (h + 1) * both)
                merged = jnp.where(wide_lane // HEAD == h, summed[piece], merged)
                c = g * 2 + h // 2
                at = inner * 4 + h % 2
                stat = st[c, r, :both]
                stat = jnp.where(lane == at, largest[piece], stat)
                st[c, r, :both] = jnp.where(lane == at + 2, total[piece], stat)
            merged = merged.astype(bf16)
            for half in range(2):
                bv[g * 2 + half, r, inner * both : (inner + 1) * both, :] = merged[
                    :, half * LANES : (half + 1) * LANES
                ]
        if groups == 1 and b < seqs - 1:
            send_piece(b)
    kept = 4 * per
    kept = -(-kept // 8) * 8
    for c in range(cols):
        for r in range(groups):
            st_part[c, r] = jnp.transpose(st[c, r])[:kept]
    st_copies = []
    for k, to in enumerate(peers):
        c, r = to // groups, lax.rem(to, groups)
        st_copies.append(remote(st_part.at[c, r], st_recv.at[k], st_s.at[k], st_r.at[k], "kv", to))
        st_copies[k].start()
    send_piece(pieces - 1)

    own = kv_part[me].astype(f32)
    for k in range(n - 1):
        kv_copies[k].wait()
        own = own + kv_recv[k].astype(f32)
    own = (own * factor).astype(bf16)
    kv_ref[me] = own
    query = q_all[me].astype(f32)
    spread = jnp.concatenate(
        [jnp.where(lane // QK == i, query, 0.0) for i in range(4)], axis=0
    ).astype(bf16)
    scores = lax.dot_general(
        spread, own[:, :LANES], (((1,), (1,)), ((), ())), preferred_element_type=f32
    )
    scores = jnp.where(lineage, scores * scale, masked_low)
    top = jnp.max(scores, axis=1, keepdims=True)
    weight = jnp.where(lineage, jnp.exp(scores - top), 0.0)
    total = jnp.sum(weight, axis=1, keepdims=True)
    summed = jnp.dot(weight.astype(bf16), own[:, LANES:], preferred_element_type=f32)

    def laid(array):
        found = []
        for b in range(per):
            for m in range(2):
                s0 = slice(m * part + b * prop, m * part + (b + 1) * prop)
                s1 = slice((2 + m) * part + b * prop, (2 + m) * part + (b + 1) * prop)
                found.append(jnp.where(low, array[s0], array[s1]))
        return jnp.concatenate(found, axis=0)

    tops, totals, sums = [laid(top)], [laid(total)], [laid(summed)]

    def take(stats, values):
        for which, into in ((0, tops), (2, totals)):
            into.append(
                jnp.concatenate(
                    [
                        jnp.where(
                            low,
                            stats[:both, b * 4 + which : b * 4 + which + 1],
                            stats[:both, b * 4 + which + 1 : b * 4 + which + 2],
                        )
                        for b in range(per)
                    ],
                    axis=0,
                )
            )
        sums.append(values.astype(f32))

    col, row = me // groups, lax.rem(me, groups)
    take(st[col, row], bv[col, row])
    filler = jnp.zeros((LANES - kept, LANES), f32)
    for copy in st_copies + b_copies:
        copy.wait()
    for k in range(n - 1):
        take(jnp.transpose(jnp.concatenate([st_recv[k], filler], axis=0)), bv_recv[k])
    highest = functools.reduce(jnp.maximum, tops)
    denominator = jnp.zeros_like(highest)
    numerator = jnp.zeros_like(highest)
    for a, b, c in zip(tops, totals, sums):
        share = jnp.exp(a - highest)
        denominator = denominator + b * share
        numerator = numerator + c * share
    attended = numerator / denominator
    heads = iota(lam_ref.shape, 1)
    lam_low = jnp.sum(jnp.where(heads == 2 * col, lam_ref[...], 0.0), axis=1, keepdims=True)
    lam_high = jnp.sum(jnp.where(heads == 2 * col + 1, lam_ref[...], 0.0), axis=1, keepdims=True)
    lam = jnp.where(low, lam_low, lam_high)
    gain = out_gain_ref[:, pl.ds(pl.multiple_of(col * LANES, LANES), LANES)]
    difference = jnp.concatenate(
        [
            attended[b * both : b * both + prop] - lam * attended[b * both + prop : (b + 1) * both]
            for b in range(per)
        ],
        axis=0,
    )
    squared = difference * difference
    one = jnp.sum(jnp.where(low, squared, 0.0), axis=1, keepdims=True)
    two = jnp.sum(jnp.where(low, 0.0, squared), axis=1, keepdims=True)
    mean = jnp.where(low, one, two) / HEAD
    norm_all[me] = (difference * lax.rsqrt(mean + epsilon) * gain).astype(bf16)
    gathers, late = [], []
    for k, to in enumerate(peers):
        gathers.append(remote(norm_all.at[me], norm_all.at[me], g_s.at[k], g_r.at[k], "kv", to))
        late.append(remote(kv_ref.at[me], kv_ref.at[me], ka_s.at[k], ka_r.at[k], "kv", to))
    for copy in gathers + late:
        copy.start()
    weights[3].wait()
    for copy in gathers:
        copy.wait()
    normed = jnp.concatenate(
        [
            jnp.concatenate([norm_all[c * groups + r] for r in range(groups)], axis=0)
            for c in range(cols)
        ],
        axis=1,
    )
    out_part[...] = jnp.dot(normed, wo_buf[...], preferred_element_type=f32).astype(bf16)
    copies = []
    for k in range(1, t):
        to = lax.rem(mine + k, t)
        copies.append(remote(out_part, out_recv.at[k], t_s.at[k], t_r.at[k], "tp", to))
    for copy in copies:
        copy.start()
    mixed = out_part[...].astype(f32)
    for k in range(1, t):
        copies[k - 1].wait()
        mixed = mixed + out_recv[k].astype(f32)
    out_ref[...] = mixed.astype(bf16)
    for copy in late:
        copy.wait()


def place_kernel(
    groups, prop, len_ref, acc_ref, kv_ref, keys_hbm, vals_hbm, nk_hbm, nv_hbm,
    kbuf, vbuf, k_in, v_in, k_out, v_out,
):
    seqs, length, width = kbuf.shape
    cols = width // LANES
    per = seqs // groups
    offset = lax.axis_index("kv") * length
    loads = []
    for b in range(seqs):
        loads.append(pltpu.make_async_copy(keys_hbm.at[b], kbuf.at[b], k_in.at[b]))
        loads.append(pltpu.make_async_copy(vals_hbm.at[b], vbuf.at[b], v_in.at[b]))
    for copy in loads:
        copy.start()
    stores = []
    window = 48
    for b in range(seqs):
        r, begin = b // per, (b % per) * prop
        rel = len_ref[b] + acc_ref[b] - offset
        base = jnp.clip((rel // 16) * 16, 0, length - window)
        at = pl.ds(pl.multiple_of(base, 16), window)
        slot = iota((window, prop), 0) + base - rel
        placing = (slot == iota((window, prop), 1)).astype(bf16)
        slot_col = iota((window, 1), 0) + base - rel
        inside = (slot_col >= 0) & (slot_col < prop)
        for which, buf in enumerate((kbuf, vbuf)):
            fresh = jnp.concatenate(
                [
                    kv_ref[c * groups + r, begin : begin + prop, which * LANES : (which + 1) * LANES]
                    for c in range(cols)
                ],
                axis=1,
            )
            moved = jnp.dot(placing, fresh, preferred_element_type=f32)
            loads[2 * b + which].wait()
            old = buf[b, at, :].astype(f32)
            buf[b, at, :] = jnp.where(inside, moved, old).astype(bf16)
            into, sem = ((nk_hbm, k_out), (nv_hbm, v_out))[which]
            stores.append(pltpu.make_async_copy(buf.at[b], into.at[b], sem.at[b]))
            stores[-1].start()
    for copy in stores:
        copy.wait()


def local(
    n, t, tokens, norm_gain, w_query, w_key, w_value, w_output, cache_keys, cache_values,
    map_lambda, out_gain, parents, lengths, accepted,
):
    rows, depth = tokens.shape
    seqs, length, width = cache_keys.shape
    prop = rows // seqs
    both = 2 * prop
    cols = min(n, width // LANES)
    groups = n // cols
    part = rows // groups
    per = seqs // groups
    pieces = seqs if groups == 1 else 1
    kept = -(-4 * per // 8) * 8
    out_cols = w_output.shape[1]
    vmem = pl.BlockSpec(memory_space=pltpu.VMEM)
    smem = pl.BlockSpec(memory_space=pltpu.SMEM)
    hbm = pl.BlockSpec(memory_space=pl.ANY)
    dma = pltpu.SemaphoreType.DMA
    V = pltpu.VMEM
    mixed, gathered = pl.pallas_call(
        functools.partial(main_kernel, n, t, cols, seqs, prop, depth * n),
        name="attend",
        out_shape=(
            jax.ShapeDtypeStruct((rows, out_cols), bf16),
            jax.ShapeDtypeStruct((n, part, 2 * LANES), bf16),
        ),
        in_specs=[vmem] * 5 + [smem] * 2 + [hbm] * 6,
        out_specs=(vmem, vmem),
        scratch_shapes=[
            V((3, depth, width), bf16),
            V(w_output.shape, bf16),
            V(cache_keys.shape, bf16),
            V(cache_values.shape, bf16),
            V((n, part, LANES), bf16),
            V((n, part, LANES), bf16),
            V((n, part, LANES), bf16),
            V((n, part, 2 * LANES), bf16),
            V((n, part, 2 * LANES), bf16),
            V((8, LANES), f32),
            V((n, 8, LANES), f32),
            V((cols, groups, per * both, LANES), bf16),
            V((n, per * both, LANES), bf16),
            V((cols, groups, LANES, LANES), f32),
            V((cols, groups, kept, LANES), f32),
            V((n, kept, LANES), f32),
            V((n, part, LANES), bf16),
            V((rows, out_cols), bf16),
            V((t, rows, out_cols), bf16),
            dma((4,)),
            dma((seqs,)),
            dma((seqs,)),
        ]
        + [dma((n,))] * 10
        + [dma((n, pieces))] * 2
        + [dma((n,))] * 4
        + [dma((t,))] * 2,
        compiler_params=pltpu.CompilerParams(collective_id=0, has_side_effects=True),
    )(
        tokens, norm_gain[None], map_lambda[None], out_gain[None], parents, lengths, accepted,
        w_query, w_key, w_value, w_output, cache_keys, cache_values,
    )
    new_keys, new_values = pl.pallas_call(
        functools.partial(place_kernel, groups, prop),
        name="place",
        out_shape=(
            jax.ShapeDtypeStruct(cache_keys.shape, bf16),
            jax.ShapeDtypeStruct(cache_values.shape, bf16),
        ),
        in_specs=[smem, smem, vmem, hbm, hbm],
        out_specs=(hbm, hbm),
        scratch_shapes=[V(cache_keys.shape, bf16), V(cache_values.shape, bf16)]
        + [dma((seqs,))] * 4,
    )(lengths, accepted, gathered, cache_keys, cache_values)
    return (mixed, new_keys, new_values)


def solution(mesh):
    placed = (
        P(None, "kv"),
        P("kv"),
        P("kv", "tp"),
        P("kv", "tp"),
        P("kv", "tp"),
        P("tp", "kv"),
        P(None, "kv", "tp"),
        P(None, "kv", "tp"),
        P("tp"),
        P("tp"),
        P(),
        P(),
        P(),
    )
    return jax.shard_map(
        functools.partial(local, mesh.shape["kv"], mesh.shape["tp"]),
        mesh=mesh,
        in_specs=placed,
        out_specs=(P(None, "kv"), P(None, "kv", "tp"), P(None, "kv", "tp")),
        check_vma=False,
    )
```

```python
import functools
import math

import jax
import jax.numpy as jnp
from jax import lax
from jax.experimental import pallas as pl
from jax.experimental.pallas import tpu as pltpu
from jax.sharding import PartitionSpec as P

HEAD = 64
QK = 32
LANES = 128
epsilon = 1e-05
masked_low = -1e30
MESH = pl.DeviceIdType.MESH
f32 = jnp.float32
bf16 = jnp.bfloat16


def iota(shape, dim):
    return lax.broadcasted_iota(jnp.int32, shape, dim)


def greet(axes):
    barrier = pltpu.get_barrier_semaphore()
    count = 0
    for axis, n in axes:
        me = lax.axis_index(axis)
        for k in range(1, n):
            pl.semaphore_signal(
                barrier, inc=1, device_id={axis: lax.rem(me + k, n)}, device_id_type=MESH
            )
            count += 1
    return barrier, count


def remote(src, dst, send_sem, recv_sem, axis, to):
    return pltpu.make_async_remote_copy(
        src_ref=src,
        dst_ref=dst,
        send_sem=send_sem,
        recv_sem=recv_sem,
        device_id={axis: to},
        device_id_type=MESH,
    )


def main_kernel(
    n, t, cols, seqs, prop, features,
    tok_ref, gain_ref, lam_ref, out_gain_ref, parent_ref, len_ref, acc_ref,
    wq_hbm, wk_hbm, wv_hbm, wo_hbm, keys_hbm, vals_hbm,
    out_ref, kv_ref,
    wbuf, wo_buf, kbuf, vbuf, q_part, q_recv, q_all, kv_part, kvx_recv, kv_sum, kvz_recv, sq_part, sq_recv,
    bv, bv_recv, st, st_part, st_recv, norm_all, out_part, out_recv,
    w_in, k_in, v_in, sq_s, sq_r, q_s, q_r, qa_s, qa_r, kx_s, kx_r, kz_s, kz_r, ax_s, ax_r, az_s, az_r,
    b_s, b_r, st_s, st_r, g_s, g_r, t_s, t_r,
):
    me = lax.axis_index("kv")
    mine = lax.axis_index("tp")
    groups = n // cols
    rows = tok_ref.shape[0]
    part = rows // groups
    per = seqs // groups
    both = 2 * prop
    _, length, width = kbuf.shape
    scale = QK ** (-0.5)
    peers = [lax.rem(me + k, n) for k in range(1, n)]
    inner_n = kv_ref.shape[0]
    outer_n = n // inner_n
    x, z = lax.rem(me, inner_n), me // inner_n
    x_peers = [lax.rem(x + k, inner_n) for k in range(1, inner_n)]
    z_peers = [lax.rem(z + k, outer_n) for k in range(1, outer_n)]
    barrier, count = greet((("kv", n), ("tp", t)))
    weights = [
        pltpu.make_async_copy(src, dst, w_in.at[i])
        for i, (src, dst) in enumerate(
            ((wq_hbm, wbuf.at[0]), (wk_hbm, wbuf.at[1]), (wv_hbm, wbuf.at[2]), (wo_hbm, wo_buf))
        )
    ]
    loads = []
    for b in range(seqs):
        loads.append(pltpu.make_async_copy(keys_hbm.at[b], kbuf.at[b], k_in.at[b]))
        loads.append(pltpu.make_async_copy(vals_hbm.at[b], vbuf.at[b], v_in.at[b]))
    for copy in weights + loads:
        copy.start()

    wide = tok_ref[...].astype(f32)
    square = jnp.sum(wide * wide, axis=1, keepdims=True)
    diagonal = iota((rows, LANES), 0) == iota((rows, LANES), 1)
    as_row = jnp.sum(jnp.where(diagonal, square, 0.0), axis=0, keepdims=True)
    sq_part[...] = jnp.broadcast_to(as_row, sq_part.shape)
    gained = (wide * gain_ref[...]).astype(bf16)

    def products(which, place):
        weights[which].wait()
        product = jnp.dot(gained, wbuf[which], preferred_element_type=f32)
        for c in range(cols):
            for r in range(groups):
                place(
                    c * groups + r,
                    product[r * part : (r + 1) * part, c * LANES : (c + 1) * LANES].astype(bf16),
                )

    def place_q(d, piece):
        q_part[d] = piece

    def place_k(d, piece):
        kv_part[d % inner_n, d // inner_n, :, :LANES] = piece

    def place_v(d, piece):
        kv_part[d % inner_n, d // inner_n, :, LANES:] = piece

    products(0, place_q)
    pl.semaphore_wait(barrier, count)
    sq_copies, q_copies = [], []
    for k, to in enumerate(peers):
        sq_copies.append(remote(sq_part, sq_recv.at[k], sq_s.at[k], sq_r.at[k], "kv", to))
        q_copies.append(remote(q_part.at[to], q_recv.at[k], q_s.at[k], q_r.at[k], "kv", to))
    for copy in sq_copies + q_copies:
        copy.start()
    products(1, place_k)
    products(2, place_v)
    kx_copies = [
        remote(kv_part.at[to], kvx_recv.at[k], kx_s.at[k], kx_r.at[k], "kv", z * inner_n + to)
        for k, to in enumerate(x_peers)
    ]
    for copy in kx_copies:
        copy.start()
    squares = sq_part[...]
    for k in range(n - 1):
        sq_copies[k].wait()
        squares = squares + sq_recv[k]
    first = lax.rem(me, groups) * part
    picked = iota((part, LANES), 0) + first == iota((part, LANES), 1)
    mean = jnp.sum(jnp.where(picked, squares[0:1], 0.0), axis=1, keepdims=True) / features
    factor = lax.rsqrt(mean + epsilon)
    total = q_part[me].astype(f32)
    for k in range(n - 1):
        q_copies[k].wait()
        total = total + q_recv[k].astype(f32)
    q_all[me] = (total * factor).astype(bf16)
    gathers = [
        remote(q_all.at[me], q_all.at[me], qa_s.at[k], qa_r.at[k], "kv", to)
        for k, to in enumerate(peers)
    ]
    for copy in gathers:
        copy.start()
    for copy in kx_copies:
        copy.wait()
    for i in range(outer_n):
        summed = kv_part[x, i].astype(f32)
        for k in range(inner_n - 1):
            summed = summed + kvx_recv[k, i].astype(f32)
        kv_sum[i] = summed.astype(bf16)
    kz_copies = [
        remote(kv_sum.at[to], kvz_recv.at[k], kz_s.at[k], kz_r.at[k], "kv", to * inner_n + x)
        for k, to in enumerate(z_peers)
    ]
    for copy in kz_copies:
        copy.start()

    lane = iota((1, LANES), 1)
    low = lane < HEAD
    own_first = lax.rem(me, groups) * per
    small_eye = iota((prop, prop), 0) == iota((prop, prop), 1)
    parent_rows = []
    for b in range(per):
        line = parent_ref[pl.ds(own_first + b, 1), :]
        parent_rows.append(
            jnp.sum(jnp.where(small_eye, line, 0), axis=1, keepdims=True)
        )
    parent = jnp.concatenate(parent_rows, axis=0)
    shape = (part, part)
    target = jnp.concatenate([p + b * prop for b, p in enumerate(parent_rows)], axis=0)
    link = (parent >= 0) & (target == iota(shape, 1))
    reach = jnp.where(link | (iota(shape, 0) == iota(shape, 1)), 1.0, 0.0)
    power = 1
    while power < prop:
        reach = jnp.minimum(
            jnp.dot(reach.astype(bf16), reach.astype(bf16), preferred_element_type=f32), 1.0
        )
        power *= 2
    lineage = jnp.concatenate([reach] * 4, axis=0) > 0.5
    st[...] = jnp.zeros_like(st)

    for copy in gathers:
        copy.wait()
    wide_lane = iota((1, 2 * LANES), 1)
    b_copies = []
    pieces = seqs if groups == 1 else 1
    tall = per * both // pieces

    def send_piece(piece):
        for k, to in enumerate(peers):
            c, r = to // groups, lax.rem(to, groups)
            span = pl.ds(piece * tall, tall)
            copy = remote(
                bv.at[c, r, span], bv_recv.at[k, span], b_s.at[k, piece], b_r.at[k, piece], "kv", to
            )
            copy.start()
            b_copies.append(copy)

    for b in range(seqs):
        r, inner = b // per, b % per
        begin = inner * prop
        rel = len_ref[b] + acc_ref[b] - me * length
        visible = iota((1, length), 1) < rel
        loads[2 * b].wait()
        loads[2 * b + 1].wait()
        for g in range(width // (2 * LANES)):
            span = slice(g * 2 * LANES, (g + 1) * 2 * LANES)
            query = jnp.concatenate(
                [
                    q_all[c * groups + r].astype(f32)[begin : begin + prop]
                    for c in (2 * g, 2 * g + 1)
                ],
                axis=1,
            )
            spread = jnp.concatenate(
                [jnp.where(wide_lane // QK == i, query, 0.0) for i in range(2 * LANES // QK)],
                axis=0,
            ).astype(bf16)
            scores = lax.dot_general(
                spread, kbuf[b, :, span], (((1,), (1,)), ((), ())), preferred_element_type=f32
            )
            scores = jnp.where(visible, scores * scale, masked_low)
            largest = jnp.max(scores, axis=1, keepdims=True)
            weight = jnp.where(visible, jnp.exp(scores - largest), 0.0)
            total = jnp.sum(weight, axis=1, keepdims=True)
            summed = jnp.dot(weight.astype(bf16), vbuf[b, :, span], preferred_element_type=f32)
            merged = jnp.zeros((both, 2 * LANES), f32)
            for h in range(2 * LANES // HEAD):
                piece = slice(h * both, (h + 1) * both)
                merged = jnp.where(wide_lane // HEAD == h, summed[piece], merged)
                c = g * 2 + h // 2
                at = inner * 4 + h % 2
                stat = st[c, r, :both]
                stat = jnp.where(lane == at, largest[piece], stat)
                st[c, r, :both] = jnp.where(lane == at + 2, total[piece], stat)
            merged = merged.astype(bf16)
            for half in range(2):
                bv[g * 2 + half, r, inner * both : (inner + 1) * both, :] = merged[
                    :, half * LANES : (half + 1) * LANES
                ]
        if groups == 1 and b < seqs - 1:
            send_piece(b)
    kept = 4 * per
    kept = -(-kept // 8) * 8
    for c in range(cols):
        for r in range(groups):
            st_part[c, r] = jnp.transpose(st[c, r])[:kept]
    st_copies = []
    for k, to in enumerate(peers):
        c, r = to // groups, lax.rem(to, groups)
        st_copies.append(remote(st_part.at[c, r], st_recv.at[k], st_s.at[k], st_r.at[k], "kv", to))
        st_copies[k].start()
    send_piece(pieces - 1)

    own = kv_sum[z].astype(f32)
    for k in range(outer_n - 1):
        kz_copies[k].wait()
        own = own + kvz_recv[k].astype(f32)
    own = (own * factor).astype(bf16)
    kv_ref[x, z] = own
    az_copies = [
        remote(kv_ref.at[x, z], kv_ref.at[x, z], az_s.at[k], az_r.at[k], "kv", to * inner_n + x)
        for k, to in enumerate(z_peers)
    ]
    for copy in az_copies:
        copy.start()
    query = q_all[me].astype(f32)
    spread = jnp.concatenate(
        [jnp.where(lane // QK == i, query, 0.0) for i in range(4)], axis=0
    ).astype(bf16)
    scores = lax.dot_general(
        spread, own[:, :LANES], (((1,), (1,)), ((), ())), preferred_element_type=f32
    )
    scores = jnp.where(lineage, scores * scale, masked_low)
    top = jnp.max(scores, axis=1, keepdims=True)
    weight = jnp.where(lineage, jnp.exp(scores - top), 0.0)
    total = jnp.sum(weight, axis=1, keepdims=True)
    summed = jnp.dot(weight.astype(bf16), own[:, LANES:], preferred_element_type=f32)

    def laid(array):
        found = []
        for b in range(per):
            for m in range(2):
                s0 = slice(m * part + b * prop, m * part + (b + 1) * prop)
                s1 = slice((2 + m) * part + b * prop, (2 + m) * part + (b + 1) * prop)
                found.append(jnp.where(low, array[s0], array[s1]))
        return jnp.concatenate(found, axis=0)

    tops, totals, sums = [laid(top)], [laid(total)], [laid(summed)]

    def take(stats, values):
        for which, into in ((0, tops), (2, totals)):
            into.append(
                jnp.concatenate(
                    [
                        jnp.where(
                            low,
                            stats[:both, b * 4 + which : b * 4 + which + 1],
                            stats[:both, b * 4 + which + 1 : b * 4 + which + 2],
                        )
                        for b in range(per)
                    ],
                    axis=0,
                )
            )
        sums.append(values.astype(f32))

    col, row = me // groups, lax.rem(me, groups)
    take(st[col, row], bv[col, row])
    filler = jnp.zeros((LANES - kept, LANES), f32)
    for copy in st_copies + b_copies:
        copy.wait()
    for k in range(n - 1):
        take(jnp.transpose(jnp.concatenate([st_recv[k], filler], axis=0)), bv_recv[k])
    highest = functools.reduce(jnp.maximum, tops)
    denominator = jnp.zeros_like(highest)
    numerator = jnp.zeros_like(highest)
    for a, b, c in zip(tops, totals, sums):
        share = jnp.exp(a - highest)
        denominator = denominator + b * share
        numerator = numerator + c * share
    attended = numerator / denominator
    heads = iota(lam_ref.shape, 1)
    lam_low = jnp.sum(jnp.where(heads == 2 * col, lam_ref[...], 0.0), axis=1, keepdims=True)
    lam_high = jnp.sum(jnp.where(heads == 2 * col + 1, lam_ref[...], 0.0), axis=1, keepdims=True)
    lam = jnp.where(low, lam_low, lam_high)
    gain = out_gain_ref[:, pl.ds(pl.multiple_of(col * LANES, LANES), LANES)]
    difference = jnp.concatenate(
        [
            attended[b * both : b * both + prop] - lam * attended[b * both + prop : (b + 1) * both]
            for b in range(per)
        ],
        axis=0,
    )
    squared = difference * difference
    one = jnp.sum(jnp.where(low, squared, 0.0), axis=1, keepdims=True)
    two = jnp.sum(jnp.where(low, 0.0, squared), axis=1, keepdims=True)
    mean = jnp.where(low, one, two) / HEAD
    norm_all[me] = (difference * lax.rsqrt(mean + epsilon) * gain).astype(bf16)
    gathers = [
        remote(norm_all.at[me], norm_all.at[me], g_s.at[k], g_r.at[k], "kv", to)
        for k, to in enumerate(peers)
    ]
    for copy in gathers:
        copy.start()
    late = [
        remote(kv_ref.at[x], kv_ref.at[x], ax_s.at[k], ax_r.at[k], "kv", z * inner_n + to)
        for k, to in enumerate(x_peers)
    ]
    for copy in az_copies:
        copy.wait()
    for copy in late:
        copy.start()
    weights[3].wait()
    for copy in gathers:
        copy.wait()
    normed = jnp.concatenate(
        [
            jnp.concatenate([norm_all[c * groups + r] for r in range(groups)], axis=0)
            for c in range(cols)
        ],
        axis=1,
    )
    out_part[...] = jnp.dot(normed, wo_buf[...], preferred_element_type=f32).astype(bf16)
    copies = []
    for k in range(1, t):
        to = lax.rem(mine + k, t)
        copies.append(remote(out_part, out_recv.at[k], t_s.at[k], t_r.at[k], "tp", to))
    for copy in copies:
        copy.start()
    mixed = out_part[...].astype(f32)
    for k in range(1, t):
        copies[k - 1].wait()
        mixed = mixed + out_recv[k].astype(f32)
    out_ref[...] = mixed.astype(bf16)
    for copy in late:
        copy.wait()


def place_kernel(
    groups, prop, len_ref, acc_ref, kv_ref, keys_hbm, vals_hbm, nk_hbm, nv_hbm,
    kbuf, vbuf, k_in, v_in, k_out, v_out,
):
    seqs, length, width = kbuf.shape
    cols = width // LANES
    per = seqs // groups
    inner_n = kv_ref.shape[0]
    offset = lax.axis_index("kv") * length
    loads = []
    for b in range(seqs):
        loads.append(pltpu.make_async_copy(keys_hbm.at[b], kbuf.at[b], k_in.at[b]))
        loads.append(pltpu.make_async_copy(vals_hbm.at[b], vbuf.at[b], v_in.at[b]))
    for copy in loads:
        copy.start()
    stores = []
    window = 48
    for b in range(seqs):
        r, begin = b // per, (b % per) * prop
        rel = len_ref[b] + acc_ref[b] - offset
        base = jnp.clip((rel // 16) * 16, 0, length - window)
        at = pl.ds(pl.multiple_of(base, 16), window)
        slot = iota((window, prop), 0) + base - rel
        placing = (slot == iota((window, prop), 1)).astype(bf16)
        slot_col = iota((window, 1), 0) + base - rel
        inside = (slot_col >= 0) & (slot_col < prop)
        for which, buf in enumerate((kbuf, vbuf)):
            fresh = jnp.concatenate(
                [
                    kv_ref[
                        (c * groups + r) % inner_n,
                        (c * groups + r) // inner_n,
                        begin : begin + prop,
                        which * LANES : (which + 1) * LANES,
                    ]
                    for c in range(cols)
                ],
                axis=1,
            )
            moved = jnp.dot(placing, fresh, preferred_element_type=f32)
            loads[2 * b + which].wait()
            old = buf[b, at, :].astype(f32)
            buf[b, at, :] = jnp.where(inside, moved, old).astype(bf16)
            into, sem = ((nk_hbm, k_out), (nv_hbm, v_out))[which]
            stores.append(pltpu.make_async_copy(buf.at[b], into.at[b], sem.at[b]))
            stores[-1].start()
    for copy in stores:
        copy.wait()


def local(
    n, t, tokens, norm_gain, w_query, w_key, w_value, w_output, cache_keys, cache_values,
    map_lambda, out_gain, parents, lengths, accepted,
):
    rows, depth = tokens.shape
    seqs, length, width = cache_keys.shape
    prop = rows // seqs
    both = 2 * prop
    cols = min(n, width // LANES)
    groups = n // cols
    part = rows // groups
    per = seqs // groups
    pieces = seqs if groups == 1 else 1
    kept = -(-4 * per // 8) * 8
    out_cols = w_output.shape[1]
    inner_n = math.gcd(n, 1 << (n.bit_length() - 1) // 2)
    outer_n = n // inner_n
    vmem = pl.BlockSpec(memory_space=pltpu.VMEM)
    smem = pl.BlockSpec(memory_space=pltpu.SMEM)
    hbm = pl.BlockSpec(memory_space=pl.ANY)
    dma = pltpu.SemaphoreType.DMA
    V = pltpu.VMEM
    mixed, gathered = pl.pallas_call(
        functools.partial(main_kernel, n, t, cols, seqs, prop, depth * n),
        name="attend",
        out_shape=(
            jax.ShapeDtypeStruct((rows, out_cols), bf16),
            jax.ShapeDtypeStruct((inner_n, outer_n, part, 2 * LANES), bf16),
        ),
        in_specs=[vmem] * 5 + [smem] * 2 + [hbm] * 6,
        out_specs=(vmem, vmem),
        scratch_shapes=[
            V((3, depth, width), bf16),
            V(w_output.shape, bf16),
            V(cache_keys.shape, bf16),
            V(cache_values.shape, bf16),
            V((n, part, LANES), bf16),
            V((n, part, LANES), bf16),
            V((n, part, LANES), bf16),
            V((inner_n, outer_n, part, 2 * LANES), bf16),
            V((inner_n, outer_n, part, 2 * LANES), bf16),
            V((outer_n, part, 2 * LANES), bf16),
            V((outer_n, part, 2 * LANES), bf16),
            V((8, LANES), f32),
            V((n, 8, LANES), f32),
            V((cols, groups, per * both, LANES), bf16),
            V((n, per * both, LANES), bf16),
            V((cols, groups, LANES, LANES), f32),
            V((cols, groups, kept, LANES), f32),
            V((n, kept, LANES), f32),
            V((n, part, LANES), bf16),
            V((rows, out_cols), bf16),
            V((t, rows, out_cols), bf16),
            dma((4,)),
            dma((seqs,)),
            dma((seqs,)),
        ]
        + [dma((n,))] * 14
        + [dma((n, pieces))] * 2
        + [dma((n,))] * 4
        + [dma((t,))] * 2,
        compiler_params=pltpu.CompilerParams(collective_id=0, has_side_effects=True),
    )(
        tokens, norm_gain[None], map_lambda[None], out_gain[None], parents, lengths, accepted,
        w_query, w_key, w_value, w_output, cache_keys, cache_values,
    )
    new_keys, new_values = pl.pallas_call(
        functools.partial(place_kernel, groups, prop),
        name="place",
        out_shape=(
            jax.ShapeDtypeStruct(cache_keys.shape, bf16),
            jax.ShapeDtypeStruct(cache_values.shape, bf16),
        ),
        in_specs=[smem, smem, vmem, hbm, hbm],
        out_specs=(hbm, hbm),
        scratch_shapes=[V(cache_keys.shape, bf16), V(cache_values.shape, bf16)]
        + [dma((seqs,))] * 4,
    )(lengths, accepted, gathered, cache_keys, cache_values)
    return (mixed, new_keys, new_values)


def solution(mesh):
    placed = (
        P(None, "kv"),
        P("kv"),
        P("kv", "tp"),
        P("kv", "tp"),
        P("kv", "tp"),
        P("tp", "kv"),
        P(None, "kv", "tp"),
        P(None, "kv", "tp"),
        P("tp"),
        P("tp"),
        P(),
        P(),
        P(),
    )
    return jax.shard_map(
        functools.partial(local, mesh.shape["kv"], mesh.shape["tp"]),
        mesh=mesh,
        in_specs=placed,
        out_specs=(P(None, "kv"), P(None, "kv", "tp"), P(None, "kv", "tp")),
        check_vma=False,
    )
```
